512 devices in a mesh: ep: 128 (over z, y, core), tp: 4 (over x).
Axes of the slice: x: 4, y: 8, z: 8, core: 2. Of those that a mesh axis runs over, the one named last changes fastest.
Arguments:
- tokens: bfloat16 [1536, 1024], P('ep'), may hold values from -6 to 6
- attention_norm_gain: bfloat16 [1024], replicated, may hold values from 0.099609375 to 1.8984375
- query_weight: bfloat16 [1024, 1024], P('ep', 'tp'), may hold values from -0.3125 to 0.3125
- key_weight: bfloat16 [1024, 256], P('ep', 'tp'), may hold values from -0.1875 to 0.1875
- value_weight: bfloat16 [1024, 256], P('ep', 'tp'), may hold values from -0.1875 to 0.1875
- per_head_gain: bfloat16 [1024], P('tp'), may hold values from 0.099609375 to 1.8984375
- lambdas: float32 [8], replicated, may hold values from 0.3 to 0.8
- output_weight: bfloat16 [1024, 1024], P('tp'), may hold values from -0.1875 to 0.1875
- key_value_cache: bfloat16 [1536, 1024, 4, 128], P('ep', None, 'tp'), may hold values from -160 to 160, as said below
- lengths: int32 [1536], P('ep'), may hold values from 1 to 1023, as said below
- expert_norm_gain: bfloat16 [1024], replicated, may hold values from 0.099609375 to 1.8984375
- routes: int32 [1536, 6], P('ep'), may hold values from 0 to 127, all different within a row; in each aligned block of 12 rows (0 to 11, 12 to 23, ...) no two rows name the same one
- routing_weight: float32 [1536, 6], P('ep'), may hold values from 0.1 to 0.6
- expert_gate_weight: bfloat16 [128, 1024, 512], P('ep', None, 'tp'), may hold values from -0.1875 to 0.1875
- expert_up_weight: bfloat16 [128, 1024, 512], P('ep', None, 'tp'), may hold values from -0.1875 to 0.1875
- expert_down_weight: bfloat16 [128, 512, 1024], P('ep', 'tp'), may hold values from -0.25 to 0.25
- dense_gate_weight: bfloat16 [1024, 256], P('ep', 'tp'), may hold values from -0.1875 to 0.1875
- dense_up_weight: bfloat16 [1024, 256], P('ep', 'tp'), may hold values from -0.1875 to 0.1875
- dense_down_weight: bfloat16 [256, 1024], P('tp'), may hold values from -0.375 to 0.375
- dense_branch_gate: bfloat16 [1024], replicated, may hold values from -0.1875 to 0.1875
Outputs:
- mixed: bfloat16 [1536, 1024], P('ep', 'tp')
- new_rows: bfloat16 [1536, 4, 128], P('ep', 'tp')
The draws below stay inside these ranges and needn't reach their ends.
Inputs may be any that keep to these rules, and one draw needn't show every extreme that they name: `key_value_cache`: cache positions at or beyond a sequence's length are never read. `lengths`: the number of cache positions already filled; the new token sits at that position; in each block of 12 sequences of one index of ep one sequence has 1023. `routes`: each row names 6 different experts; among the rows of one index of ep no expert is named more than 1 times, a bound that some block reaches.
All inputs are finite; a program needn't handle non-finite values.
Results may differ from the reference program's by a relative error of at most 0.015.
The reference program's roundings to bfloat16 on the way count: a program that leaves them out, or rounds other values in their place, can miss the bound.
Values may be sent and summed in bfloat16 or wider, within the bound.
A program may use at most 64 MiB of HBM per device.

```python
import math
import jax
import jax.numpy as jnp
import numpy as np
from jax import lax

MODEL_DIM = 1024
HEADS = 8
KV_HEADS = 2
HD = 64
VD = 128
EXPERT_HIDDEN = 512
FS = 256
TOP = 6
CACHE = 1024
SEQ_DEV = 12
SEQS = 1536
ROUTED_EXPERTS = 128
CAP = 1
N_EP = 128
N_TP = 4


def draw_key_value_cache(key, part):
    values = jax.random.normal(key, (SEQS, CACHE, 2 * KV_HEADS, HD + VD // 2), jnp.float32)
    values = jnp.clip(values, -4.0, 4.0)
    return values.astype(jnp.bfloat16)


def draw_lengths(key, part):
    first_key, second_key = jax.random.split(key)
    base = jax.random.randint(first_key, (SEQS,), 1, CACHE)
    chosen = jax.random.randint(second_key, (SEQS // SEQ_DEV,), 0, SEQ_DEV)
    owner = jnp.arange(SEQS) // SEQ_DEV
    marked = jnp.arange(SEQS) % SEQ_DEV == chosen[owner]
    return jnp.where(marked, CACHE - 1, base).astype(jnp.int32)


def shard_levels(stream_key, extent, pieces, least, top_value):
    def one(axis_at, blocks):
        heights = jax.random.uniform(jax.random.fold_in(jax.random.fold_in(stream_key, 6), axis_at), (blocks,), jnp.float32, least / len(pieces), top_value / len(pieces))
        return jnp.repeat(jnp.exp(heights), extent[axis_at] // blocks).reshape((-1,) + (1,) * (len(extent) - axis_at - 1))

    level = one(*pieces[0])
    for cut in pieces[1:]:
        level = level * one(*cut)
    return level


def assign_block(own_key, own, number, rows, number_of, top, limit, slope):
    ranking = jax.random.permutation(own_key, number_of)
    crowded, common = portions_of(number_of, rows * top, limit, slope, True), portions_of(number_of, rows * top, limit, slope, False)
    places = jnp.arange(number_of)

    def named(sizes, turn):
        used = int((sizes > 0).sum())
        fixed = max(1, used // 4)
        passed = fixed + (places - fixed + turn * (used - fixed)) % max(1, number_of - fixed)
        return jnp.zeros((number_of,), jnp.int32).at[ranking[jnp.where(places < fixed, places, passed)]].set(jnp.asarray(sizes, jnp.int32))

    sizes = jnp.where(number % 4 == 0, named(crowded, number // 4), named(common, number - number // 4 - 1))
    mixed = jax.random.permutation(jax.random.fold_in(own, 3), number_of)
    source_of, sink = mixed[0:number_of // 2 * 2:2], mixed[1:number_of // 2 * 2:2]
    slack = jnp.minimum(sizes[source_of] - 1, limit - sizes[sink]) // 2
    slack = jnp.where((source_of == ranking[0]) | (sink == ranking[0]) | (sizes[sink] == 0), 0, jnp.maximum(slack, 0))
    passed = jax.random.randint(jax.random.fold_in(own, 4), (number_of // 2,), 0, 1 << 20) % (slack + 1)
    sizes = sizes.at[source_of].add(-passed).at[sink].add(passed)
    labels = jnp.searchsorted(jnp.cumsum(sizes), jnp.arange(rows * top), side="right").astype(jnp.int32)
    listing = labels.reshape(top, rows).T
    listing = listing[jax.random.permutation(jax.random.fold_in(own, 1), rows)]
    turn = jax.random.randint(jax.random.fold_in(own, 2), (rows, 1), 0, top)
    return jnp.take_along_axis(listing, (jnp.arange(top)[None, :] + turn) % top, axis=1)


def portions_of(number_of, total, reach, slope, full):
    portions = [(1 << 20) // math.isqrt(grade ** slope) + 1 for grade in range(1, number_of + 1)]
    largest = reach if full else min(reach, max(-(-total // number_of), total * portions[0] // sum(portions)))
    least = 1 if total - largest >= number_of - 1 else 0
    given, rest = [largest] + [least] * (number_of - 1), total - largest - least * (number_of - 1)
    while rest > 0:
        candidates = [i for i in range(1, number_of) if given[i] < largest] or [i for i in range(1, number_of) if given[i] < reach]
        whole, left = sum([portions[i] for i in candidates]), rest
        for i in candidates:
            more = min(reach - given[i], max(1, left * portions[i] // whole), rest)
            given[i] = given[i] + more
            rest = rest - more
    return np.array(given)


def noise(key, dims, scale, reach, cuts=(), kind=jnp.bfloat16):
    result = scale * jax.random.normal(key, dims, jnp.float32)
    if cuts:
        result = result * shard_levels(key, dims, cuts, -0.22, 0.18)
    return jnp.clip(result, -reach, reach).astype(kind)


def setup_inputs(seed: int = 0) -> dict:
    key_list = jax.random.split(jax.random.key(seed), 21)
    tokens = noise(key_list[0], (SEQS, MODEL_DIM), 1.0, 6.0, ((0, 128),))
    attention_norm_gain = jnp.clip(1.0 + 0.18 * jax.random.normal(key_list[1], (MODEL_DIM,), jnp.float32), 0.099609375, 1.8984375).astype(jnp.bfloat16)
    query_weight = noise(key_list[2], (MODEL_DIM, 2 * HD * HEADS), (MODEL_DIM // 3) ** -0.5, 0.3125, ((0, 128), (1, 4)))
    key_weight = noise(key_list[3], (MODEL_DIM, 2 * HD * KV_HEADS), MODEL_DIM ** -0.5, 0.1875, ((0, 128), (1, 4)))
    value_weight = noise(key_list[4], (MODEL_DIM, VD * KV_HEADS), MODEL_DIM ** -0.5, 0.1875, ((0, 128), (1, 4)))
    per_head_gain = jnp.clip(1.0 + 0.18 * jax.random.normal(key_list[5], (HEADS * VD,), jnp.float32), 0.099609375, 1.8984375).astype(jnp.bfloat16)
    lambdas = jnp.clip(jax.random.uniform(key_list[6], (HEADS,), jnp.float32, 0.3, 0.8), 0.3, 0.8)
    output_weight = noise(key_list[7], (HEADS * VD, MODEL_DIM), (HEADS * VD) ** -0.5, 0.1875, ((0, 4),))
    key_value_cache = draw_key_value_cache(jax.random.fold_in(key_list[20], 71), 0)
    lengths = draw_lengths(jax.random.fold_in(key_list[20], 71), 0)
    expert_norm_gain = jnp.clip(1.0 + 0.18 * jax.random.normal(key_list[10], (MODEL_DIM,), jnp.float32), 0.099609375, 1.8984375).astype(jnp.bfloat16)
    routes_keys = jax.random.split(jax.random.fold_in(key_list[11], 1), SEQS // SEQ_DEV)
    routes_turns = jax.random.permutation(jax.random.fold_in(key_list[11], 3), SEQS // SEQ_DEV)
    routes = jax.vmap(lambda own, number: assign_block(jax.random.fold_in(key_list[11], 2), own, number, SEQ_DEV, ROUTED_EXPERTS, TOP, CAP, 2))(routes_keys, routes_turns).reshape((SEQS, TOP))
    routing_weight = jnp.clip(0.1 + 0.5 * jax.random.uniform(key_list[12], (SEQS, TOP), jnp.float32) ** shard_levels(key_list[12], (SEQS, TOP), ((0, 128),), -0.2, 0.2), 0.1, 0.6)
    expert_gate_weight = noise(key_list[13], (ROUTED_EXPERTS, MODEL_DIM, EXPERT_HIDDEN), MODEL_DIM ** -0.5, 0.1875, ((0, 128), (2, 4)))
    expert_up_weight = noise(key_list[14], (ROUTED_EXPERTS, MODEL_DIM, EXPERT_HIDDEN), MODEL_DIM ** -0.5, 0.1875, ((0, 128), (2, 4)))
    expert_down_weight = noise(key_list[15], (ROUTED_EXPERTS, EXPERT_HIDDEN, MODEL_DIM), EXPERT_HIDDEN ** -0.5, 0.25, ((0, 128), (1, 4)))
    dense_gate_weight = noise(key_list[16], (MODEL_DIM, FS), MODEL_DIM ** -0.5, 0.1875, ((0, 128), (1, 4)))
    dense_up_weight = noise(key_list[17], (MODEL_DIM, FS), MODEL_DIM ** -0.5, 0.1875, ((0, 128), (1, 4)))
    dense_down_weight = noise(key_list[18], (FS, MODEL_DIM), FS ** -0.5, 0.375, ((0, 4),))
    dense_branch_gate = noise(key_list[19], (MODEL_DIM,), MODEL_DIM ** -0.5, 0.1875)
    return dict(tokens=tokens, attention_norm_gain=attention_norm_gain, query_weight=query_weight, key_weight=key_weight, value_weight=value_weight, per_head_gain=per_head_gain, lambdas=lambdas, output_weight=output_weight, key_value_cache=key_value_cache, lengths=lengths, expert_norm_gain=expert_norm_gain, routes=routes, routing_weight=routing_weight, expert_gate_weight=expert_gate_weight, expert_up_weight=expert_up_weight, expert_down_weight=expert_down_weight, dense_gate_weight=dense_gate_weight, dense_up_weight=dense_up_weight, dense_down_weight=dense_down_weight, dense_branch_gate=dense_branch_gate)


epsilon = 1e-06

def rms_scale(values, gain):
    mean_sq = lax.optimization_barrier(jnp.mean(values * values, axis=-1, keepdims=True))
    return values * lax.rsqrt(mean_sq + epsilon) * gain.astype(jnp.float32)

def softmax_map(query, key_new, keys, seq_lengths):
    span = keys.shape[1]
    scale = query.shape[-1] ** (-0.5)
    query_f = query.astype(jnp.float32)
    scores = jnp.einsum('skgd,sckd->skgc', query_f, keys.astype(jnp.float32)) * scale
    own = jnp.einsum('skgd,skd->skg', query_f, key_new.astype(jnp.float32)) * scale
    live = jnp.arange(span)[None, :] < seq_lengths[:, None]
    scores = jnp.where(live[:, None, None, :], scores, -jnp.inf)
    peak = jnp.maximum(lax.optimization_barrier(jnp.max(scores, axis=-1)), own)
    weights = jnp.exp(scores - peak[..., None])
    own_weight = jnp.exp(own - peak)
    total = lax.optimization_barrier(jnp.sum(weights, axis=-1)) + own_weight
    return (weights / total[..., None], own_weight / total)

def reference(tokens, attention_norm_gain, query_weight, key_weight, value_weight, per_head_gain, lambdas, output_weight, key_value_cache, lengths, expert_norm_gain, routes, routing_weight, expert_gate_weight, expert_up_weight, expert_down_weight, dense_gate_weight, dense_up_weight, dense_down_weight, dense_branch_gate):
    normed = rms_scale(tokens.astype(jnp.float32), attention_norm_gain).astype(jnp.bfloat16)
    query = jnp.dot(normed, query_weight, preferred_element_type=jnp.float32).astype(jnp.bfloat16)
    key_new = jnp.dot(normed, key_weight, preferred_element_type=jnp.float32).astype(jnp.bfloat16)
    value_new = jnp.dot(normed, value_weight, preferred_element_type=jnp.float32).astype(jnp.bfloat16)
    group = HEADS // KV_HEADS
    half = VD // 2
    query_b = query.reshape(N_EP, SEQ_DEV, 2, KV_HEADS, group, HD)
    key_b = key_new.reshape(N_EP, SEQ_DEV, 2, KV_HEADS, HD)
    value_b = value_new.reshape(N_EP, SEQ_DEV, 2, KV_HEADS, half)
    cache_b = key_value_cache.reshape(N_EP, SEQ_DEV, CACHE, 2, KV_HEADS, HD + half)
    length_b = lengths.reshape(N_EP, SEQ_DEV)
    lam = lambdas.reshape(KV_HEADS, group)
    gain = per_head_gain.reshape(2, KV_HEADS, group, half).astype(jnp.float32)

    def one_block(items):
        q_blk, k_blk, v_blk, c_blk, l_blk = items
        first_w, first_own = softmax_map(q_blk[:, 0], k_blk[:, 0], c_blk[:, :, 0, :, :HD], l_blk)
        second_w, second_own = softmax_map(q_blk[:, 1], k_blk[:, 1], c_blk[:, :, 1, :, :HD], l_blk)
        mixed_weights = (first_w - lam[None, :, :, None] * second_w).astype(jnp.bfloat16)
        mixed_own = (first_own - lam[None] * second_own).astype(jnp.bfloat16)
        values = c_blk[..., HD:].astype(jnp.float32)
        heads = jnp.einsum('skgc,schkv->shkgv', mixed_weights.astype(jnp.float32), values)
        heads = heads + mixed_own.astype(jnp.float32)[:, None, :, :, None] * v_blk.astype(jnp.float32)[:, :, :, None, :]
        sums = lax.optimization_barrier(jnp.sum(heads * heads, axis=(1, 4), keepdims=True))
        return (heads * lax.rsqrt(sums / VD + epsilon) * gain[None]).astype(jnp.bfloat16)
    heads = lax.map(one_block, (query_b, key_b, value_b, cache_b, length_b))
    heads_flat = heads.reshape(SEQS, HEADS * VD)
    block = HEADS * VD // N_TP
    attn_out = jnp.zeros((SEQS, MODEL_DIM), jnp.float32)
    for member in range(N_TP):
        piece = jnp.dot(heads_flat[:, member * block:(member + 1) * block], output_weight[member * block:(member + 1) * block], preferred_element_type=jnp.float32)
        attn_out = attn_out + lax.optimization_barrier(piece.astype(jnp.bfloat16)).astype(jnp.float32)
    resid = tokens.astype(jnp.float32) + attn_out
    normed_ffn = rms_scale(resid, expert_norm_gain).astype(jnp.bfloat16)
    dense_gate = jnp.dot(normed_ffn, dense_gate_weight, preferred_element_type=jnp.float32)
    dense_up = jnp.dot(normed_ffn, dense_up_weight, preferred_element_type=jnp.float32)
    dense_hidden = (jax.nn.silu(dense_gate) * dense_up).astype(jnp.bfloat16)
    dense_out = jnp.dot(dense_hidden, dense_down_weight, preferred_element_type=jnp.float32)
    gate = jax.nn.sigmoid(jnp.dot(normed_ffn, dense_branch_gate, preferred_element_type=jnp.float32))
    expert_flat = routes.reshape(-1).astype(jnp.int32)
    token_flat = jnp.repeat(jnp.arange(SEQS, dtype=jnp.int32), TOP)
    quarter = EXPERT_HIDDEN // N_TP

    def one_route(pair):
        expert_index, token_row = pair
        source_rows = normed_ffn[token_row]
        gate_part = jnp.dot(source_rows, expert_gate_weight[expert_index], preferred_element_type=jnp.float32)
        up_projected = jnp.dot(source_rows, expert_up_weight[expert_index], preferred_element_type=jnp.float32)
        inner = (jax.nn.silu(gate_part) * up_projected).astype(jnp.bfloat16)
        down = expert_down_weight[expert_index]
        summed = jnp.zeros((MODEL_DIM,), jnp.float32)
        for member in range(N_TP):
            piece = jnp.dot(inner[member * quarter:(member + 1) * quarter], down[member * quarter:(member + 1) * quarter], preferred_element_type=jnp.float32)
            summed = summed + lax.optimization_barrier(piece.astype(jnp.bfloat16)).astype(jnp.float32)
        return summed.astype(jnp.bfloat16)
    expert_out = lax.map(one_route, (expert_flat, token_flat)).reshape(SEQS, TOP, MODEL_DIM)
    routed = lax.optimization_barrier(jnp.sum(routing_weight[..., None] * expert_out.astype(jnp.float32), axis=1))
    mixed = (resid + routed + gate[:, None] * dense_out).astype(jnp.bfloat16)
    new_rows = jnp.concatenate([key_new.reshape(SEQS, 2, KV_HEADS, HD), value_new.reshape(SEQS, 2, KV_HEADS, half)], axis=3)
    return (mixed, new_rows.reshape(SEQS, 2 * KV_HEADS, HD + half))
```

```python
import functools

import jax
import jax.numpy as jnp
from jax import lax
from jax.experimental import pallas as pl
from jax.experimental.pallas import tpu as pltpu
from jax.sharding import Mesh
from jax.sharding import PartitionSpec as P

HD = 64
VD = 128
EP = ("ep_0", "ep_1", "ep_2")


epsilon = 1e-06


def sent_to_all(x, axis):
    copies = jnp.broadcast_to(x, (lax.axis_size(axis), *x.shape))
    return lax.all_to_all(copies, axis, split_axis=0, concat_axis=0, tiled=True)


def in_order(pieces, dim):
    pieces = jnp.moveaxis(pieces, 0, dim)
    dims = pieces.shape
    return pieces.reshape(*dims[:dim], dims[dim] * dims[dim + 1], *dims[dim + 2 :])


def gathered_by_axis(x, axes, dim):
    far, near = axes
    pieces = sent_to_all(sent_to_all(x, far), near)
    return in_order(pieces.swapaxes(0, 1).reshape(-1, *x.shape), dim)


def from_partner(block, axis, bit):
    count = lax.axis_size(axis)
    route = []
    for low in range(count):
        high = low | 1 << bit
        if high != low and high < count:
            route += [(low, high), (high, low)]
    return lax.ppermute(block, axis, route)


def over_copies(x, axis):
    return sent_to_all(x, axis).astype(jnp.float32).sum(axis=0)


def in_blocks(x, dim, count):
    dims = x.shape
    pieces = x.reshape(*dims[:dim], count, dims[dim] // count, *dims[dim + 1 :])
    return jnp.moveaxis(pieces, dim, 0)


def summed_on_arrival(x, axis, dim):
    count = lax.axis_size(axis)
    pieces = lax.all_to_all(in_blocks(x, dim, count), axis, 0, 0, tiled=True)
    return jnp.sum(pieces.astype(jnp.float32), axis=0)


MESH_ID = pl.DeviceIdType.MESH


def exchange_kernel(nz, ny, nc, src, dst, send_sem, recv_sem):
    z, y, c = (lax.axis_index(name) for name in EP)
    x = lax.axis_index("tp")
    count = nz * ny * nc
    me = (z * ny + y) * nc + c

    def peer(k):
        i, j, dc = k // (ny * nc), (k // nc) % ny, k % nc
        dz = nz // 2 + (1 - 2 * (i % 2)) * ((i + 1) // 2)
        dy = ny // 2 + (1 - 2 * (j % 2)) * ((j + 1) // 2)
        z2, y2, c2 = (z + dz) % nz, (y + dy) % ny, (c + dc + 1) % nc
        return (z2 * ny + y2) * nc + c2, (z2, y2, c2, x)

    barrier = pltpu.get_barrier_semaphore()

    def greet(k, carry):
        pl.semaphore_signal(barrier, inc=1, device_id=peer(k)[1], device_id_type=MESH_ID)
        return carry

    lax.fori_loop(0, count - 1, greet, 0)
    dst[me] = src[me]
    pl.semaphore_wait(barrier, count - 1)

    def send(k, carry):
        other, device = peer(k)
        pltpu.make_async_remote_copy(
            src.at[other], dst.at[me], send_sem, recv_sem, device_id=device, device_id_type=MESH_ID
        ).start()
        return carry

    lax.fori_loop(0, count - 1, send, 0)
    rest = pl.ds(0, count - 1)
    pltpu.make_async_copy(src.at[rest], dst.at[rest], recv_sem).wait()
    pltpu.make_async_copy(src.at[rest], dst.at[rest], send_sem).wait()


def exchange(rows, collective_id):
    nz, ny, nc = (lax.axis_size(name) for name in EP)
    return pl.pallas_call(
        functools.partial(exchange_kernel, nz, ny, nc),
        out_shape=jax.ShapeDtypeStruct(rows.shape, rows.dtype),
        in_specs=[pl.BlockSpec(memory_space=pltpu.VMEM)],
        out_specs=pl.BlockSpec(memory_space=pltpu.VMEM),
        scratch_shapes=[pltpu.SemaphoreType.DMA, pltpu.SemaphoreType.DMA],
        compiler_params=pltpu.CompilerParams(collective_id=collective_id, has_side_effects=True),
    )(rows)


def rms_scale(values, gain):
    mean_sq = jnp.mean(values * values, axis=-1, keepdims=True)
    return values * lax.rsqrt(mean_sq + epsilon) * gain.astype(jnp.float32)


def project(normed, weight):
    return jnp.dot(
        normed,
        gathered_by_axis(weight, (("ep_0", "ep_1"), "ep_2"), 0),
        preferred_element_type=jnp.float32,
    )


def map_weights(query, key_new, keys, seq_lengths):
    span = keys.shape[1]
    scale = query.shape[-1] ** (-0.5)
    scores = jnp.einsum("sugd,scud->sugc", query, keys, preferred_element_type=jnp.float32) * scale
    own = jnp.einsum("sugd,sud->sug", query, key_new, preferred_element_type=jnp.float32) * scale
    live = jnp.arange(span)[None, :] < seq_lengths[:, None]
    scores = jnp.where(live[:, None, None, :], scores, -jnp.inf)
    peak = jnp.maximum(jnp.max(scores, axis=-1), own)
    weights = jnp.exp(scores - peak[..., None])
    own_weight = jnp.exp(own - peak)
    total = jnp.sum(weights, axis=-1) + own_weight
    return (weights / total[..., None], own_weight / total)


def per_device(
    tokens,
    attention_norm_gain,
    query_weight,
    key_weight,
    value_weight,
    per_head_gain,
    lambdas,
    output_weight,
    key_value_cache,
    lengths,
    expert_norm_gain,
    routes,
    routing_weight,
    expert_gate_weight,
    expert_up_weight,
    expert_down_weight,
    dense_gate_weight,
    dense_up_weight,
    dense_down_weight,
    dense_branch_gate,
):
    sequences, model_width = tokens.shape
    units = key_value_cache.shape[2]
    lanes = key_value_cache.shape[3]
    normed = rms_scale(tokens.astype(jnp.float32), attention_norm_gain).astype(jnp.bfloat16)
    joined = jnp.concatenate([query_weight, key_weight, value_weight], axis=1)
    projected = project(normed, joined).astype(jnp.bfloat16)
    query_width = query_weight.shape[1]
    key_width = key_weight.shape[1]
    query = projected[:, :query_width].reshape(sequences, units, -1, HD)
    key_new = projected[:, query_width : query_width + key_width].reshape(sequences, units, HD)
    value_new = projected[:, query_width + key_width :].reshape(sequences, units, lanes - HD)
    weights, own_weight = map_weights(query, key_new, key_value_cache[..., :HD], lengths)
    members = lax.axis_size("tp")
    partner_bit = members.bit_length() - 2
    other, other_own = (
        from_partner(weights.astype(jnp.bfloat16), "tp", partner_bit).astype(weights.dtype),
        from_partner(own_weight.astype(jnp.bfloat16), "tp", partner_bit).astype(own_weight.dtype),
    )
    position = lax.axis_index("tp")
    first_map = position < members // 2
    kv_count = units * members // 2
    kv_ids = (position * units + jnp.arange(units, dtype=jnp.int32)) % kv_count
    table = lambdas.reshape(kv_count, -1)
    matches = kv_ids[:, None, None] == jnp.arange(kv_count, dtype=jnp.int32)[None, :, None]
    lam = jnp.sum(jnp.where(matches, table[None], 0.0), axis=1)
    leading = jnp.where(first_map, weights, other)
    trailing = jnp.where(first_map, other, weights)
    lead_own = jnp.where(first_map, own_weight, other_own)
    trail_own = jnp.where(first_map, other_own, own_weight)
    mixed_weights = (leading - lam[None, :, :, None] * trailing).astype(jnp.bfloat16)
    mixed_own = (lead_own - lam[None] * trail_own).astype(jnp.bfloat16)
    heads = jnp.einsum(
        "sugc,scuv->sugv",
        mixed_weights,
        key_value_cache[..., HD:],
        preferred_element_type=jnp.float32,
    )
    heads = (
        heads
        + mixed_own.astype(jnp.float32)[..., None] * value_new.astype(jnp.float32)[:, :, None, :]
    )
    squares = jnp.sum(heads * heads, axis=-1)
    partner_squares = from_partner(squares, "tp", partner_bit)
    scaling = lax.rsqrt((squares + partner_squares) / VD + epsilon)
    gain = per_head_gain.reshape(units, -1, lanes - HD).astype(jnp.float32)
    heads_normed = (heads * scaling[..., None] * gain[None]).astype(jnp.bfloat16)
    partial_value = jnp.dot(
        heads_normed.reshape(sequences, -1), output_weight, preferred_element_type=jnp.float32
    )
    attn_out = over_copies(partial_value.astype(jnp.bfloat16), "tp").astype(jnp.float32)
    resid = tokens.astype(jnp.float32) + attn_out
    normed_ffn = rms_scale(resid, expert_norm_gain).astype(jnp.bfloat16)
    dense_in = project(normed_ffn, jnp.concatenate([dense_gate_weight, dense_up_weight], axis=1))
    hidden_units = dense_gate_weight.shape[1]
    dense_hidden = (jax.nn.silu(dense_in[:, :hidden_units]) * dense_in[:, hidden_units:]).astype(
        jnp.bfloat16
    )
    dense_part = jnp.dot(dense_hidden, dense_down_weight, preferred_element_type=jnp.float32)
    dense_out = summed_on_arrival(dense_part.astype(jnp.bfloat16), "tp", 1)
    gate = jax.nn.sigmoid(
        jnp.dot(normed_ffn, dense_branch_gate, preferred_element_type=jnp.float32)
    )
    expert_count = lax.axis_size(EP)
    top_count = routes.shape[1]
    capacity = (sequences * top_count + expert_count - 1) // expert_count
    named = routes[:, :, None] == jnp.arange(expert_count, dtype=jnp.int32)[None, None, :]
    hits = jnp.sum(named.astype(jnp.int32), axis=1)
    before = jnp.cumsum(hits, axis=0) - hits
    slot_of = jnp.sum(jnp.where(named, before[:, None, :], 0), axis=2)
    placing = (hits[:, :, None] > 0) & (
        before[:, :, None] == jnp.arange(capacity, dtype=jnp.int32)[None, None, :]
    )
    outgoing = jnp.einsum(
        "sec,sd->ecd", placing.astype(jnp.bfloat16), normed_ffn, preferred_element_type=jnp.float32
    ).astype(jnp.bfloat16)
    arrived = exchange(outgoing.reshape(expert_count, 8, -1), 0).reshape(outgoing.shape)
    sources, count, features = arrived.shape
    flattened_rows = arrived.reshape(sources * count, features)
    gate_part = jnp.dot(flattened_rows, expert_gate_weight[0], preferred_element_type=jnp.float32)
    up_projected = jnp.dot(flattened_rows, expert_up_weight[0], preferred_element_type=jnp.float32)
    inner = (jax.nn.silu(gate_part) * up_projected).astype(jnp.bfloat16)
    outcome = jnp.dot(inner, expert_down_weight[0], preferred_element_type=jnp.float32)
    quarter = summed_on_arrival(outcome.astype(jnp.bfloat16), "tp", 1).astype(jnp.bfloat16)
    quarter = quarter.reshape(sources, count, -1)
    answers = exchange(quarter.reshape(expert_count, 2, -1), 1).reshape(quarter.shape)
    quarter_width = answers.shape[2]
    answer_rows = answers.reshape(expert_count * capacity, quarter_width)
    picked = answer_rows[routes * capacity + slot_of]
    routed = jnp.sum(routing_weight[..., None] * picked.astype(jnp.float32), axis=1)
    column_start = lax.axis_index("tp") * quarter_width
    resid_part = lax.dynamic_slice_in_dim(resid, column_start, quarter_width, 1)
    mixed = (resid_part + routed + gate[:, None] * dense_out).astype(jnp.bfloat16)
    new_rows = jnp.concatenate([key_new, value_new], axis=2)
    return (mixed, new_rows)


def solution(mesh):
    split = Mesh(mesh.devices.reshape(8, 8, 2, mesh.shape["tp"]), ("ep_0", "ep_1", "ep_2", "tp"))
    return jax.shard_map(
        per_device,
        mesh=split,
        in_specs=(
            P(EP, None),
            P(),
            P(EP, "tp"),
            P(EP, "tp"),
            P(EP, "tp"),
            P("tp"),
            P(),
            P("tp", None),
            P(EP, None, "tp", None),
            P(EP),
            P(),
            P(EP, None),
            P(EP, None),
            P(EP, None, "tp"),
            P(EP, None, "tp"),
            P(EP, "tp", None),
            P(EP, "tp"),
            P(EP, "tp"),
            P("tp", None),
            P(),
        ),
        out_specs=(P(EP, "tp"), P(EP, "tp", None)),
        check_vma=False,
    )
```
